32 devices in a mesh: ra: 4 (over z), cb: 4 (over y, x), dp: 2 (over core).
Axes of the slice: x: 2, y: 2, z: 4, core: 2. Of those that a mesh axis runs over, the one named last changes fastest.
Arguments:
- stream: bfloat16 [4, 64, 4096], P('dp', None, 'ra'), may hold values from -16 to 16
- norm_gain: bfloat16 [2, 4096], P(None, 'ra'), may hold values from 0.099609375 to 1.8984375
- gate_weight: bfloat16 [2, 4096, 12288], P(None, 'ra', 'cb'), may hold values from -0.09375 to 0.09375
- value_weight: bfloat16 [2, 4096, 12288], P(None, 'ra', 'cb'), may hold values from -0.09375 to 0.09375
- gate_taps: bfloat16 [2, 3, 12288], P(None, None, 'cb'), may hold values from -3 to 3
- value_taps: bfloat16 [2, 3, 12288], P(None, None, 'cb'), may hold values from -3 to 3
- gate_bias: bfloat16 [2, 12288], P(None, 'cb'), may hold values from -3 to 3
- value_bias: bfloat16 [2, 12288], P(None, 'cb'), may hold values from -3 to 3
- down_weight: bfloat16 [2, 12288, 4096], P(None, 'cb', 'ra'), may hold values from -0.0546875 to 0.0546875
- final_gain: bfloat16 [4096], P('ra'), may hold values from 0.099609375 to 1.8984375
Outputs:
- mixed: bfloat16 [4, 64, 4096], P('dp', None, 'ra')
The draws below stay inside these ranges and needn't reach their ends.
All inputs are finite; a program needn't handle non-finite values.
Results may differ from the reference program's by a relative error of at most 0.035.
Values may be sent and summed in bfloat16 or wider, within the bound.
A program may use at most 128 MiB of HBM per device.

```python
import jax
import jax.numpy as jnp
from jax import lax

D = 4096
FF = 12288
TAPS = 3
LAYERS = 2
LEN = 64
BATCH = 4
N_CB = 4


def draw_stream(key, part):
    first, second, third = jax.random.split(key, 3)
    base = jnp.clip(jax.random.normal(first, (BATCH, LEN, D), jnp.float32), -4.0, 4.0)
    channel = jnp.exp(jax.random.uniform(second, (D // 16,), jnp.float32, -1.1, 1.1))
    rowscale = jnp.exp(jax.random.uniform(third, (BATCH, LEN), jnp.float32, -0.7, 0.7))
    values = base * jnp.repeat(channel, 16)[None, None, :] * rowscale[:, :, None]
    return jnp.clip(values, -16.0, 16.0).astype(jnp.bfloat16)


def steps_of(rng, extent, cuts, smallest, largest):
    def one(position, blocks):
        heights = jax.random.uniform(jax.random.fold_in(jax.random.fold_in(rng, 6), position), (blocks,), jnp.float32, smallest / len(cuts), largest / len(cuts))
        return jnp.repeat(jnp.exp(heights), extent[position] // blocks).reshape((-1,) + (1,) * (len(extent) - position - 1))

    gain = one(*cuts[0])
    for cut in cuts[1:]:
        gain = gain * one(*cut)
    return gain


def bell_draw(stream_key, shape, spread, most, shards=(), kind=jnp.bfloat16):
    values = spread * jax.random.normal(stream_key, shape, jnp.float32)
    if shards:
        values = values * steps_of(stream_key, shape, shards, -0.22, 0.18)
    return jnp.clip(values, -most, most).astype(kind)


def setup_inputs(seed: int = 0) -> dict:
    keys = jax.random.split(jax.random.key(seed), 11)
    stream = draw_stream(jax.random.fold_in(keys[10], 71), 0)
    norm_gain = jnp.clip(1.0 + 0.18 * jax.random.normal(keys[1], (LAYERS, D), jnp.float32), 0.099609375, 1.8984375).astype(jnp.bfloat16)
    gate_weight = bell_draw(keys[2], (LAYERS, D, FF), D ** -0.5, 0.09375, ((1, 4), (2, 4)))
    value_weight = bell_draw(keys[3], (LAYERS, D, FF), D ** -0.5, 0.09375, ((1, 4), (2, 4)))
    gate_taps = bell_draw(keys[4], (LAYERS, TAPS, FF), 0.577, 3.0, ((2, 4),))
    value_taps = bell_draw(keys[5], (LAYERS, TAPS, FF), 0.577, 3.0, ((2, 4),))
    gate_bias = bell_draw(keys[6], (LAYERS, FF), 0.5, 3.0, ((1, 4),))
    value_bias = bell_draw(keys[7], (LAYERS, FF), 0.5, 3.0, ((1, 4),))
    down_weight = bell_draw(keys[8], (LAYERS, FF, D), FF ** -0.5, 0.0546875, ((1, 4), (2, 4)))
    final_gain = jnp.clip(1.0 + 0.18 * jax.random.normal(keys[9], (D,), jnp.float32), 0.099609375, 1.8984375).astype(jnp.bfloat16)
    return dict(stream=stream, norm_gain=norm_gain, gate_weight=gate_weight, value_weight=value_weight, gate_taps=gate_taps, value_taps=value_taps, gate_bias=gate_bias, value_bias=value_bias, down_weight=down_weight, final_gain=final_gain)


EPS = 1e-06

def rms_scaled(stream_in, gain_row):
    values = stream_in.astype(jnp.float32)
    squares = lax.optimization_barrier(jnp.sum(values * values, axis=-1, keepdims=True))
    return values * lax.rsqrt(squares / D + EPS) * gain_row.astype(jnp.float32)

def causal_mix(up_rows, taps, bias):
    length = up_rows.shape[1]
    count = taps.shape[0]
    padded = jnp.pad(up_rows.astype(jnp.float32), ((0, 0), (count - 1, 0), (0, 0)))
    result = jnp.zeros(up_rows.shape, jnp.float32) + bias.astype(jnp.float32)
    for tap_index in range(count):
        result = result + padded[:, tap_index:tap_index + length] * taps[tap_index].astype(jnp.float32)
    return result

def reference(stream, norm_gain, gate_weight, value_weight, gate_taps, value_taps, gate_bias, value_bias, down_weight, final_gain):
    batch_rows, length, width = stream.shape
    current = stream
    ff_block = FF // N_CB
    for layer_index in range(LAYERS):
        normed = rms_scaled(current, norm_gain[layer_index]).astype(jnp.bfloat16).reshape(-1, width)
        gate_up = jnp.dot(normed, gate_weight[layer_index], preferred_element_type=jnp.float32).astype(jnp.bfloat16)
        value_up = jnp.dot(normed, value_weight[layer_index], preferred_element_type=jnp.float32).astype(jnp.bfloat16)
        gate_conv = causal_mix(gate_up.reshape(batch_rows, length, FF), gate_taps[layer_index], gate_bias[layer_index])
        value_conv = causal_mix(value_up.reshape(batch_rows, length, FF), value_taps[layer_index], value_bias[layer_index])
        hidden = (jax.nn.gelu(gate_conv) * value_conv).astype(jnp.bfloat16).reshape(-1, FF)
        branch = jnp.zeros((hidden.shape[0], width), jnp.float32)
        for block_index in range(N_CB):
            lower = block_index * ff_block
            term = jnp.dot(hidden[:, lower:lower + ff_block], down_weight[layer_index, lower:lower + ff_block], preferred_element_type=jnp.float32)
            rounded = lax.optimization_barrier(term.astype(jnp.bfloat16))
            branch = branch + rounded.astype(jnp.float32)
        current = (0.5 * current.astype(jnp.float32) + branch.reshape(batch_rows, length, width)).astype(jnp.bfloat16)
    return rms_scaled(current, final_gain).astype(jnp.bfloat16)
```

```python
import functools

import jax
import jax.numpy as jnp
from jax import lax
from jax.experimental import pallas as pl
from jax.experimental.pallas import tpu as pltpu
from jax.sharding import PartitionSpec as P

EPS = 1e-06
MESH = pl.DeviceIdType.MESH
LANES = 128
UNITS = 256
SKEW = 3
SKEW_BACK = 2
OWN_LAG = 3
NEXT_LAG = 7
END_LAG = 3
UP, MIX = 0, 1


def chain_kernel(
    dims,
    s_in, ng, gt, vt, gb, vb, fg, wg_hbm, wv_hbm, dn_hbm,
    out,
    w, dn, u, part, rs_send, rs_recv, hid, acc, scale, coef,
    sq_send, sq_recv, tbuf, rbuf, snew, sfin, fsq_send, fsq_recv, fin,
    wsem, dsem, p_ss, p_rs, rs_ss, rs_rs, ag_ss, ag_rs, sq_ss, sq_rs,
    t_ss, t_rs, n_ss, n_rs, i_ss, i_rs, fs_ss, fs_rs, f_ss, f_rs,
):
    n, m, width = dims
    layers, _, chunks, dl, cw2 = w.shape
    cw = cw2 // 2
    groups, rows = hid.shape[1], hid.shape[4]
    half = groups // 2
    rq = rows // m
    taps = gt.shape[0]
    me = lax.axis_index("ra")
    mc = lax.axis_index("cb")
    core = lax.axis_index("dp")
    f32, bf16 = jnp.float32, jnp.bfloat16
    items = groups * chunks
    off_owner = SKEW * (n - 2)
    off_down = off_owner + SKEW_BACK * (n - 1)
    off_own = off_down + OWN_LAG
    off_end = off_own + END_LAG
    period = max(items, chunks + off_own + NEXT_LAG)

    def place(lane):
        return jnp.where(lane == 1, me, n - 1 - me)

    def wcopy(l, lane, c, which):
        src = (wg_hbm, wv_hbm)[which]
        cols = pl.ds(pl.multiple_of((lane * chunks + c) * cw, LANES), cw)
        return pltpu.make_async_copy(
            src.at[l, :, cols], w.at[l, lane, c, :, pl.ds(which * cw, cw)], wsem.at[l, lane, c, which]
        )

    def dcopy(l, lane, c):
        units = pl.ds(pl.multiple_of((lane * chunks + c) * cw, LANES), cw)
        return pltpu.make_async_copy(dn_hbm.at[l, units, :], dn.at[l, lane, c], dsem.at[l, lane, c])

    def remote(src, dst, ss, rs, **to):
        return pltpu.make_async_remote_copy(
            src_ref=src, dst_ref=dst, send_sem=ss, recv_sem=rs, device_id=to, device_id_type=MESH
        )

    def toward(lane, back):
        step = jnp.where((lane == 1) != back, 1, n - 1)
        return lax.rem(me + step, n)

    def own(q):
        return pl.ds(pl.multiple_of(q * rq, rq), rq)

    def part_copy(l, h, lane, c):
        return remote(
            part.at[h, lane, c], part.at[h, lane, c], p_ss.at[l, h, lane, c], p_rs.at[l, h, lane, c], dp=MIX
        )

    def rs_copy(l, h, lane, c):
        return remote(
            rs_send.at[l, h, lane, c], rs_recv.at[l, h, lane, c],
            rs_ss.at[l, h, lane, c], rs_rs.at[l, h, lane, c], ra=toward(lane, False), dp=MIX,
        )

    def ag_copy(l, h, lane, c):
        return remote(
            hid.at[l, h, lane, c], hid.at[l, h, lane, c],
            ag_ss.at[l, h, lane, c], ag_rs.at[l, h, lane, c], ra=toward(lane, True), dp=MIX,
        )

    def sq_copy(l, h, e):
        return remote(
            sq_send.at[l, h], sq_recv.at[l, h, me], sq_ss.at[l, h, e], sq_rs.at[l, h, me],
            ra=(0, n - 1)[e], dp=MIX,
        )

    def sq_wait(l, h, r):
        remote(
            sq_send.at[l, h], sq_recv.at[l, h, r], sq_ss.at[l, h, 0], sq_rs.at[l, h, r], ra=me, dp=MIX
        ).wait_recv()

    def t_copy(l, h, o):
        to = lax.rem(mc + o, m)
        return remote(tbuf.at[l, h, own(to)], rbuf.at[l, h, o], t_ss.at[l, h, o], t_rs.at[l, h, o], cb=to)

    def n_copy(l, h, o):
        mine = own(mc)
        return remote(
            snew.at[l, h, mine], snew.at[l, h, mine], n_ss.at[l, h, o], n_rs.at[l, h, o],
            cb=lax.rem(mc + o, m), dp=UP,
        )

    def n_wait(l, h, o):
        theirs = own(lax.rem(mc + m - o, m))
        remote(
            snew.at[l, h, theirs], snew.at[l, h, theirs], n_ss.at[l, h, o], n_rs.at[l, h, o],
            cb=lax.rem(mc + o, m), dp=UP,
        ).wait_recv()

    def full_copy(h):
        return remote(
            s_in.at[pl.ds((h - half) * rows, rows)], snew.at[0, h], i_ss.at[h], i_rs.at[h], dp=UP
        )

    def mine_copy(h):
        return remote(
            s_in.at[pl.ds(pl.multiple_of(h * rows + mc * rq, rq), rq)], snew.at[0, h, own(mc)],
            i_ss.at[h], i_rs.at[h], dp=MIX,
        )

    def fsq_copy(h, o):
        return remote(
            fsq_send.at[h], fsq_recv.at[h, o], fs_ss.at[h, o], fs_rs.at[h, o], ra=lax.rem(me + o, n)
        )

    def out_rows(h, q):
        return pl.ds(pl.multiple_of(lax.rem(h, half) * rows + q * rq, rq), rq)

    def f_copy(h, o):
        return remote(
            fin.at[h], out.at[out_rows(h, mc)], f_ss.at[h, o], f_rs.at[h, o],
            cb=lax.rem(mc + o, m), dp=h // half,
        )

    def f_wait(h, o):
        remote(
            fin.at[h], out.at[out_rows(h, lax.rem(mc + m - o, m))], f_ss.at[h, o], f_rs.at[h, o],
            cb=lax.rem(mc + o, m), dp=h // half,
        ).wait_recv()

    @pl.when(core == UP)
    def _():
        for c in range(chunks):
            for lane in range(2):
                for which in range(2):
                    wcopy(0, lane, c, which).start()

    @pl.when(core == MIX)
    def _():
        for c in range(chunks):
            for lane in range(2):
                dcopy(0, lane, c).start()

    barrier = pltpu.get_barrier_semaphore()
    for o in range(n):
        for other in range(2):
            if o or other:
                pl.semaphore_signal(
                    barrier, inc=1, device_id={"ra": lax.rem(me + o, n), "dp": lax.rem(core + other, 2)},
                    device_id_type=MESH,
                )
    for o in range(1, m):
        for other in range(2):
            pl.semaphore_signal(
                barrier, inc=1, device_id={"cb": lax.rem(mc + o, m), "dp": lax.rem(core + other, 2)},
                device_id_type=MESH,
            )

    @pl.when(core == UP)
    def _():
        for h in range(half):
            snew[0, h] = s_in[h * rows : (h + 1) * rows]

    @pl.when(core == MIX)
    def _():
        mine = own(mc)
        for h in range(half, groups):
            snew[0, h, mine] = s_in[pl.ds(pl.multiple_of((h - half) * rows + mc * rq, rq), rq)]
        acc[...] = jnp.zeros(acc.shape, f32)
        lane = jnp.where(me == 0, 0, 1)
        for l in range(layers):
            for c in range(chunks):
                cols = pl.ds(pl.multiple_of((lane * chunks + c) * cw, LANES), cw)
                for i in range(taps):
                    coef[l, c, i : i + 1] = gt[i, l : l + 1, cols].astype(f32)
                    coef[l, c, taps + 1 + i : taps + 2 + i] = vt[i, l : l + 1, cols].astype(f32)
                coef[l, c, taps : taps + 1] = gb[l : l + 1, cols].astype(f32)
                coef[l, c, 2 * taps + 1 : 2 * taps + 2] = vb[l : l + 1, cols].astype(f32)

    pl.semaphore_wait(barrier, 2 * n - 1 + 2 * (m - 1))

    @pl.when(core == UP)
    def _():
        for h in range(half):
            mine_copy(h).start()

        first = jnp.where(me == 0, 1, 0)

        def item(i, carry):
            l = i // items
            rest = i - l * items
            h = rest // chunks
            c = rest - h * chunks

            @pl.when(c == 0)
            def _():
                @pl.when((l == 0) & (h >= half))
                def _():
                    full_copy(h).wait_recv()

                @pl.when(l > 0)
                def _():
                    for o in range(m):
                        n_wait(l, h, o)

                gain = ng[0:1, :].astype(f32)
                for x in range(1, layers):
                    gain = jnp.where(l == x, ng[x : x + 1, :].astype(f32), gain)
                u[...] = (snew[l, h].astype(f32) * gain).astype(bf16)

            @pl.when(h == 0)
            def _():
                for lane in range(2):
                    for which in range(2):
                        wcopy(l, lane, c, which).wait()

            for a in range(2):
                lane = first if a == 0 else 1 - first
                k = place(lane)

                def up():
                    return jnp.dot(u[...], w[l, lane, c], preferred_element_type=f32)

                if a == 0:

                    @pl.when(k == 0)
                    def _():
                        rs_send[l, h, lane, c] = up().astype(bf16)
                        rs_copy(l, h, lane, c).start()

                @pl.when(k > 0)
                def _():
                    @pl.when(l > 0)
                    def _():
                        part_copy(l - 1, h, lane, c).wait_send()

                    part[h, lane, c] = up()
                    part_copy(l, h, lane, c).start()

            @pl.when(c == 0)
            def _():
                values = snew[l, h].astype(f32)
                total = jnp.sum(values * values, axis=1, keepdims=True)
                square = jnp.broadcast_to(jnp.concatenate([total] * (LANES // rows), axis=0), (LANES, LANES))
                sq_send[l, h] = square.T[0:8]
                for e in range(2):
                    sq_copy(l, h, e).start()

            @pl.when(i == chunks - 1)
            def _():
                for x in range(1, layers):
                    for cc in range(chunks):
                        for lane in range(2):
                            for which in range(2):
                                wcopy(x, lane, cc, which).start()

            return carry

        lax.fori_loop(0, layers * items, item, 0)

        for h in range(half):
            for o in range(m):
                f_wait(h, o)

        def drain(i, carry):
            l = i // items
            rest = i - l * items
            h = rest // chunks
            c = rest - h * chunks
            for lane in range(2):
                k = place(lane)

                @pl.when(k == 0)
                def _():
                    rs_copy(l, h, lane, c).wait_send()

                @pl.when((k > 0) & (l == layers - 1))
                def _():
                    part_copy(l, h, lane, c).wait_send()

            return carry

        lax.fori_loop(0, layers * items, drain, 0)
        for h in range(half):
            mine_copy(h).wait_send()
        for l in range(layers):
            for h in range(groups):
                for e in range(2):
                    sq_copy(l, h, e).wait_send()

    @pl.when(core == MIX)
    def _():
        for h in range(half, groups):
            full_copy(h).start()

        position = lax.broadcasted_iota(jnp.int32, (rows, cw), 0)

        def mix(x, rest, at):
            result = rest[at + taps : at + taps + 1] + x * rest[at + taps - 1 : at + taps]
            for back in range(1, taps):
                moved = jnp.where(position >= back, pltpu.roll(x, back, 0), 0.0)
                result = result + moved * rest[at + taps - 1 - back : at + taps - back]
            return result

        def finish_scale(l, h):
            total = jnp.zeros((8, LANES), f32)
            for r in range(n):
                sq_wait(l, h, r)
                total = total + sq_recv[l, h, r]
            inverse = lax.rsqrt(total / width + EPS)
            scale[...] = jnp.broadcast_to(inverse[0:1], (LANES, LANES)).T[0:rows]

        def split(i):
            at = jnp.maximum(i, 0)
            l = at // period
            rest = at - l * period
            valid = (i >= 0) & (l < layers) & (rest < items)
            l = jnp.minimum(l, layers - 1)
            rest = jnp.minimum(rest, items - 1)
            h = rest // chunks
            return valid, l, h, rest - h * chunks

        def step(t, carry):
            for lane in range(2):
                k = place(lane)
                valid, l, h, c = split(t - SKEW * (k - 1))

                @pl.when(valid & (k > 0))
                def _():
                    part_copy(l, h, lane, c).wait_recv()
                    rs_copy(l, h, lane, c).wait_recv()

                    @pl.when(k < n - 1)
                    def _():
                        rs_send[l, h, lane, c] = (part[h, lane, c] + rs_recv[l, h, lane, c].astype(f32)).astype(bf16)
                        rs_copy(l, h, lane, c).start()

                    @pl.when(k == n - 1)
                    def _():
                        @pl.when(c == 0)
                        def _():
                            finish_scale(l, h)

                        factor = jnp.concatenate([scale[...]] * (cw // LANES), axis=1)
                        rest = coef[l, c]
                        gate = (part[h, lane, c, :, :cw] + rs_recv[l, h, lane, c, :, :cw].astype(f32)) * factor
                        value = (part[h, lane, c, :, cw:] + rs_recv[l, h, lane, c, :, cw:].astype(f32)) * factor
                        gate = mix(gate, rest, 0)
                        value = mix(value, rest, taps + 1)
                        hid[l, h, lane, c] = (jax.nn.gelu(gate) * value).astype(bf16)
                        ag_copy(l, h, lane, c).start()

            for lane in range(2):
                k = place(lane)
                valid, l, h, c = split(t - off_owner - SKEW_BACK * (n - 1 - k))

                @pl.when(valid & (k < n - 1))
                def _():
                    ag_copy(l, h, lane, c).wait_recv()

                    @pl.when(k > 0)
                    def _():
                        ag_copy(l, h, lane, c).start()

            valid, l, h, c = split(t - off_own)

            @pl.when(valid & (c == chunks - 1))
            def _():
                mine = own(mc)

                @pl.when((l == 0) & (h < half))
                def _():
                    mine_copy(h).wait_recv()

                total = tbuf[l, h, mine].astype(f32)
                for o in range(1, m):
                    t_copy(l, h, o).wait_recv()
                    total = total + rbuf[l, h, o].astype(f32)
                new = (0.5 * snew[l, h, mine].astype(f32) + total).astype(bf16)

                @pl.when(l < layers - 1)
                def _():
                    snew[l + 1, h, mine] = new
                    for o in range(m):
                        n_copy(l + 1, h, o).start()

                @pl.when(l == layers - 1)
                def _():
                    sfin[h] = new
                    values = new.astype(f32)
                    fsq_send[h] = jnp.broadcast_to(jnp.sum(values * values, axis=1, keepdims=True), (rq, LANES))
                    for o in range(1, n):
                        fsq_copy(h, o).start()

            valid, l, h, c = split(t - off_down)

            @pl.when(valid)
            def _():
                @pl.when(h == 0)
                def _():
                    for lane in range(2):
                        dcopy(l, lane, c).wait()

                acc[...] += jnp.dot(hid[l, h, 0, c], dn[l, 0, c], preferred_element_type=f32) + jnp.dot(
                    hid[l, h, 1, c], dn[l, 1, c], preferred_element_type=f32
                )

                @pl.when(c == chunks - 1)
                def _():
                    tbuf[l, h] = acc[...].astype(bf16)
                    for o in range(1, m):
                        t_copy(l, h, o).start()
                    acc[...] = jnp.zeros(acc.shape, f32)

            valid, l, h, c = split(t - off_end)

            @pl.when(valid & (c == chunks - 1) & (l == layers - 1))
            def _():
                total = fsq_send[h]
                for o in range(1, n):
                    fsq_copy(h, o).wait_recv()
                    total = total + fsq_recv[h, o]
                factor = jnp.concatenate([lax.rsqrt(total / width + EPS)] * (dl // LANES), axis=1)
                fin[h] = (sfin[h].astype(f32) * factor * fg[...].astype(f32).reshape(1, dl)).astype(bf16)

                @pl.when(h < half)
                def _():
                    f_copy(h, 0).start()

                for o in range(1, m):
                    f_copy(h, o).start()

                @pl.when(h >= half)
                def _():
                    out[out_rows(h, mc)] = fin[h]

            @pl.when(t == chunks - 1)
            def _():
                for x in range(1, layers):
                    for cc in range(chunks):
                        for lane in range(2):
                            dcopy(x, lane, cc).start()

            return carry

        lax.fori_loop(0, (layers - 1) * period + items + off_end, step, 0)

        for h in range(half, groups):
            for o in range(1, m):
                f_wait(h, o)

        def drain(i, carry):
            l = i // items
            rest = i - l * items
            h = rest // chunks
            c = rest - h * chunks
            for lane in range(2):
                k = place(lane)

                @pl.when((k > 0) & (k < n - 1))
                def _():
                    rs_copy(l, h, lane, c).wait_send()

                @pl.when(k > 0)
                def _():
                    ag_copy(l, h, lane, c).wait_send()

            return carry

        lax.fori_loop(0, layers * items, drain, 0)
        for h in range(half, groups):
            full_copy(h).wait_send()
        for h in range(groups):
            for l in range(layers):
                for o in range(1, m):
                    t_copy(l, h, o).wait_send()
                if l:
                    for o in range(m):
                        n_copy(l, h, o).wait_send()
            for o in range(1, n):
                fsq_copy(h, o).wait_send()
            for o in range(0 if h < half else 1, m):
                f_copy(h, o).wait_send()


def body(n, m, width, stream, norm_gain, gate_weight, value_weight, gate_taps, value_taps,
         gate_bias, value_bias, down_weight, final_gain):
    batch, length, dl = stream.shape
    layers, _, ff = gate_weight.shape
    taps = gate_taps.shape[1]
    groups, rows = 2 * batch, length
    cw = UNITS
    chunks = ff // 2 // cw
    rq = rows // m
    bf16, f32 = jnp.bfloat16, jnp.float32
    vmem = pl.BlockSpec(memory_space=pltpu.VMEM)
    hbm = pl.BlockSpec(memory_space=pl.ANY)
    dma = pltpu.SemaphoreType.DMA
    pieces = (layers, groups, 2, chunks)
    result = pl.pallas_call(
        functools.partial(chain_kernel, (n, m, width)),
        out_shape=jax.ShapeDtypeStruct((batch * length, dl), bf16),
        in_specs=[vmem] * 7 + [hbm] * 3,
        out_specs=vmem,
        scratch_shapes=[
            pltpu.VMEM((layers, 2, chunks, dl, 2 * cw), bf16),
            pltpu.VMEM((layers, 2, chunks, cw, dl), bf16),
            pltpu.VMEM((rows, dl), bf16),
            pltpu.VMEM((groups, 2, chunks, rows, 2 * cw), f32),
            pltpu.VMEM(pieces + (rows, 2 * cw), bf16),
            pltpu.VMEM(pieces + (rows, 2 * cw), bf16),
            pltpu.VMEM(pieces + (rows, cw), bf16),
            pltpu.VMEM((rows, dl), f32),
            pltpu.VMEM((rows, LANES), f32),
            pltpu.VMEM((layers, chunks, -(-(2 * taps + 2) // 8) * 8, cw), f32),
            pltpu.VMEM((layers, groups, 8, LANES), f32),
            pltpu.VMEM((layers, groups, n, 8, LANES), f32),
            pltpu.VMEM((layers, groups, rows, dl), bf16),
            pltpu.VMEM((layers, groups, m, rq, dl), bf16),
            pltpu.VMEM((layers, groups, rows, dl), bf16),
            pltpu.VMEM((groups, rq, dl), bf16),
            pltpu.VMEM((groups, rq, LANES), f32),
            pltpu.VMEM((groups, n, rq, LANES), f32),
            pltpu.VMEM((groups, rq, dl), bf16),
            dma((layers, 2, chunks, 2)),
            dma((layers, 2, chunks)),
            dma(pieces), dma(pieces), dma(pieces), dma(pieces), dma(pieces), dma(pieces),
            dma((layers, groups, 2)), dma((layers, groups, n)),
            dma((layers, groups, m)), dma((layers, groups, m)),
            dma((layers, groups, m)), dma((layers, groups, m)),
            dma((groups,)), dma((groups,)),
            dma((groups, n)), dma((groups, n)),
            dma((groups, m)), dma((groups, m)),
        ],
        compiler_params=pltpu.CompilerParams(
            collective_id=0, has_side_effects=True, vmem_limit_bytes=67_000_000
        ),
    )(
        stream.reshape(batch * length, dl), norm_gain, gate_taps.swapaxes(0, 1), value_taps.swapaxes(0, 1),
        gate_bias, value_bias, final_gain, gate_weight, value_weight, down_weight,
    )
    return result.reshape(batch, length, dl)


def solution(mesh):
    n, m = mesh.shape["ra"], mesh.shape["cb"]

    def run(stream, *rest):
        specs = (
            P("dp", None, "ra"),
            P(None, "ra"),
            P(None, "ra", "cb"),
            P(None, "ra", "cb"),
            P(None, None, "cb"),
            P(None, None, "cb"),
            P(None, "cb"),
            P(None, "cb"),
            P(None, "cb", "ra"),
            P("ra"),
        )
        return jax.shard_map(
            functools.partial(body, n, m, stream.shape[2]),
            mesh=mesh, in_specs=specs, out_specs=P("dp", None, "ra"), check_vma=False,
        )(stream, *rest)

    return run
```

```python
import functools

import jax
import jax.numpy as jnp
from jax import lax
from jax.experimental import pallas as pl
from jax.experimental.pallas import tpu as pltpu
from jax.sharding import PartitionSpec as P

EPS = 1e-06
MESH = pl.DeviceIdType.MESH
LANES = 128
UNITS = 256
SKEW = 3
SKEW_BACK = 2
OWN_LAG = 3
NEXT_LAG = 5
END_LAG = 4
LAST_BACK = 0
OWN_EXTRA = 1
UP, MIX = 0, 1


def chain_kernel(
    dims,
    s_in, ng, gt, vt, gb, vb, fg, wg_hbm, wv_hbm, dn_hbm,
    out,
    w, dn, u, part, rs_send, rs_recv, hid, acc, scale, coef,
    sq_send, sq_recv, tbuf, rbuf, snew, fin, raw, fsq_send, fsq_recv,
    wsem, dsem, p_ss, rs_ss, rs_rs, ag_ss, ag_rs, sq_ss, sq_rs,
    t_ss, t_rs, n_ss, n_rs, i_ss, i_rs, fs_ss, fs_rs, f_ss, f_rs,
):
    n, m, width = dims
    layers, chunks, _, dl, cw2 = w.shape
    cw = cw2 // 2
    groups, rows = hid.shape[1], hid.shape[4]
    half = groups // 2
    rq = rows // m
    taps = gt.shape[0]
    me = lax.axis_index("ra")
    mc = lax.axis_index("cb")
    core = lax.axis_index("dp")
    f32, bf16 = jnp.float32, jnp.bfloat16
    items = groups * chunks
    off_owner = SKEW * (n - 2)
    off_down = off_owner + SKEW_BACK * (n - 1)
    off_own = off_down + OWN_LAG
    off_end = off_own + END_LAG
    period = max(items + OWN_EXTRA, chunks + off_own + NEXT_LAG)

    def place(lane):
        return jnp.where(lane == 1, me, n - 1 - me)

    def wcopy(l, lane, c, which):
        src = (wg_hbm, wv_hbm)[which]
        cols = pl.ds(pl.multiple_of((lane * chunks + c) * cw, LANES), cw)
        return pltpu.make_async_copy(
            src.at[l, :, cols], w.at[l, c, lane, :, pl.ds(which * cw, cw)], wsem.at[l, c]
        )

    def dcopy(l, lane, c):
        units = pl.ds(pl.multiple_of((lane * chunks + c) * cw, LANES), cw)
        return pltpu.make_async_copy(dn_hbm.at[l, units, :], dn.at[l, c, lane], dsem.at[l, c])

    def remote(src, dst, ss, rs, **to):
        return pltpu.make_async_remote_copy(
            src_ref=src, dst_ref=dst, send_sem=ss, recv_sem=rs, device_id=to, device_id_type=MESH
        )

    def toward(lane, back):
        step = jnp.where((lane == 1) != back, 1, n - 1)
        return lax.rem(me + step, n)

    def own(q):
        return pl.ds(pl.multiple_of(q * rq, rq), rq)

    def part_copy(l, h, lane, c):
        return remote(
            part.at[h, lane, c], part.at[h, lane, c], p_ss.at[l, h, lane], rs_rs.at[h, lane, c], dp=MIX
        )

    def rs_copy(l, h, lane, c):
        return remote(
            rs_send.at[l, h, lane, c], rs_recv.at[l, h, lane, c],
            rs_ss.at[l, h, lane], rs_rs.at[h, lane, c], ra=toward(lane, False), dp=MIX,
        )

    def ag_copy(l, h, lane, c):
        return remote(
            hid.at[l, h, lane, c], hid.at[l, h, lane, c],
            ag_ss.at[l, h, lane], ag_rs.at[h, lane, c], ra=toward(lane, True), dp=MIX,
        )

    def sq_copy(l, h, e):
        return remote(
            sq_send.at[l, h], sq_recv.at[l, h, me], sq_ss.at[l, h, e], sq_rs.at[l, h],
            ra=(0, n - 1)[e], dp=MIX,
        )

    def t_copy(l, h, o):
        to = lax.rem(mc + o, m)
        return remote(tbuf.at[l, h, own(to)], rbuf.at[l, h, o], t_ss.at[l, h], t_rs.at[l, h], cb=to)

    def n_copy(l, h, o):
        mine = own(mc)
        return remote(
            snew.at[l, h, mine], snew.at[l, h, mine], n_ss.at[l, h], n_rs.at[l, h],
            cb=lax.rem(mc + o, m), dp=UP,
        )

    def full_copy(h):
        return remote(
            s_in.at[pl.ds((h - half) * rows, rows)], snew.at[0, h], i_ss.at[h], i_rs.at[h], dp=UP
        )

    def mine_copy(h):
        return remote(
            s_in.at[pl.ds(pl.multiple_of(h * rows + mc * rq, rq), rq)], snew.at[0, h, own(mc)],
            i_ss.at[h], i_rs.at[h], dp=MIX,
        )

    def fsq_copy(h, r, o):
        return remote(
            fsq_send.at[h], fsq_recv.at[lax.rem(h, half), me * m + mc], fs_ss.at[h], fs_rs.at[h],
            ra=lax.rem(me + r, n), cb=lax.rem(mc + o, m), dp=h // half,
        )

    def f_copy(h, o):
        return remote(
            fin.at[h], raw.at[lax.rem(h, half), own(mc)], f_ss.at[h], f_rs.at[h],
            cb=lax.rem(mc + o, m), dp=h // half,
        )

    def arrived(ref, sem):
        remote(ref, ref, f_ss.at[0], sem, dp=core).wait_recv()

    def left(ref, sem):
        remote(ref, ref, sem, f_rs.at[0], dp=core).wait_send()

    def end(h):
        at = lax.rem(h, half)
        for q in range(m):
            total = fsq_recv[at, q]
            for r in range(1, n):
                total = total + fsq_recv[at, r * m + q]
            inverse = lax.rsqrt(total / width + EPS)
            factor = jnp.broadcast_to(inverse, (LANES, LANES)).T[0:rq]
            factor = jnp.concatenate([factor] * (dl // LANES), axis=1)
            scaled = raw[at, q * rq : (q + 1) * rq].astype(f32) * factor * fg[...].astype(f32).reshape(1, dl)
            out[pl.ds(pl.multiple_of(at * rows + q * rq, rq), rq)] = scaled.astype(bf16)

    barrier = pltpu.get_barrier_semaphore()

    def greet(**to):
        pl.semaphore_signal(barrier, inc=1, device_id=to, device_id_type=MESH)

    @pl.when(core == UP)
    def _():
        for o in range(m):
            greet(cb=lax.rem(mc + o, m), dp=MIX)

    @pl.when(core == MIX)
    def _():
        for o in range(n):
            greet(ra=lax.rem(me + o, n), dp=UP)
        for o in range(1, n):
            greet(ra=lax.rem(me + o, n), dp=MIX)
        for o in range(1, m):
            greet(cb=lax.rem(mc + o, m), dp=MIX)

    @pl.when(core == UP)
    def _():
        for c in range(chunks):
            for lane in range(2):
                for which in range(2):
                    wcopy(0, lane, c, which).start()

    @pl.when(core == MIX)
    def _():
        for c in range(chunks):
            for lane in range(2):
                dcopy(0, lane, c).start()

    @pl.when(core == UP)
    def _():
        for h in range(half):
            snew[0, h] = s_in[h * rows : (h + 1) * rows]

    @pl.when(core == MIX)
    def _():
        mine = own(mc)
        for h in range(half, groups):
            snew[0, h, mine] = s_in[pl.ds(pl.multiple_of((h - half) * rows + mc * rq, rq), rq)]
        acc[...] = jnp.zeros(acc.shape, f32)
        lane = jnp.where(me == 0, 0, 1)
        for l in range(layers):
            for c in range(chunks):
                cols = pl.ds(pl.multiple_of((lane * chunks + c) * cw, LANES), cw)
                for i in range(taps):
                    coef[l, c, i : i + 1] = gt[i, l : l + 1, cols].astype(f32)
                    coef[l, c, taps + 1 + i : taps + 2 + i] = vt[i, l : l + 1, cols].astype(f32)
                coef[l, c, taps : taps + 1] = gb[l : l + 1, cols].astype(f32)
                coef[l, c, 2 * taps + 1 : 2 * taps + 2] = vb[l : l + 1, cols].astype(f32)

    @pl.when(core == UP)
    def _():
        pl.semaphore_wait(barrier, n)
        for h in range(half):
            mine_copy(h).start()

        first = jnp.where(me == 0, 1, 0)

        def item(i, carry):
            l = i // items
            rest = i - l * items
            h = rest // chunks
            c = rest - h * chunks

            @pl.when(c == 0)
            def _():
                @pl.when((l == 0) & (h >= half))
                def _():
                    full_copy(h).wait_recv()

                @pl.when(l > 0)
                def _():
                    arrived(snew.at[l, h], n_rs.at[l, h])

                gain = ng[0:1, :].astype(f32)
                for x in range(1, layers):
                    gain = jnp.where(l == x, ng[x : x + 1, :].astype(f32), gain)
                u[...] = (snew[l, h].astype(f32) * gain).astype(bf16)

            @pl.when(h == 0)
            def _():
                pltpu.make_async_copy(w.at[l, c], w.at[l, c], wsem.at[l, c]).wait()

            for a in range(2):
                lane = first if a == 0 else 1 - first
                k = place(lane)

                def up():
                    return jnp.dot(u[...], w[l, c, lane], preferred_element_type=f32)

                if a == 0:

                    @pl.when(k == 0)
                    def _():
                        rs_send[l, h, lane, c] = up().astype(bf16)
                        rs_copy(l, h, lane, c).start()

                @pl.when(k > 0)
                def _():
                    @pl.when((l > 0) & (c == 0))
                    def _():
                        left(part.at[h, lane], p_ss.at[l - 1, h, lane])

                    part[h, lane, c] = up()
                    part_copy(l, h, lane, c).start()

            @pl.when(c == 0)
            def _():
                values = snew[l, h].astype(f32)
                total = jnp.sum(values * values, axis=1, keepdims=True)
                square = jnp.broadcast_to(jnp.concatenate([total] * (LANES // rows), axis=0), (LANES, LANES))
                sq_send[l, h] = square.T[0:8]
                for e in range(2):
                    sq_copy(l, h, e).start()

            @pl.when(i == chunks - 1)
            def _():
                for x in range(1, layers):
                    for cc in range(chunks):
                        for lane in range(2):
                            for which in range(2):
                                wcopy(x, lane, cc, which).start()

            return carry

        lax.fori_loop(0, layers * items, item, 0)

        for h in range(groups):
            for lane in range(2):
                k = place(lane)

                @pl.when(k == 0)
                def _():
                    for l in range(layers):
                        left(rs_send.at[l, h, lane], rs_ss.at[l, h, lane])

                @pl.when(k > 0)
                def _():
                    left(part.at[h, lane], p_ss.at[layers - 1, h, lane])

            for l in range(layers):
                for e in range(2):
                    sq_copy(l, h, e).wait_send()
        for h in range(half):
            mine_copy(h).wait_send()
        for h in range(half):
            arrived(raw.at[h], f_rs.at[h])
            arrived(fsq_recv.at[h], fs_rs.at[h])
            end(h)

    @pl.when(core == MIX)
    def _():
        pl.semaphore_wait(barrier, n + 2 * m - 2)
        for h in range(half, groups):
            full_copy(h).start()

        position = lax.broadcasted_iota(jnp.int32, (rows, cw), 0)

        def mix(x, rest, at):
            result = rest[at + taps : at + taps + 1] + x * rest[at + taps - 1 : at + taps]
            for back in range(1, taps):
                moved = jnp.where(position >= back, pltpu.roll(x, back, 0), 0.0)
                result = result + moved * rest[at + taps - 1 - back : at + taps - back]
            return result

        def finish_scale(l, h):
            arrived(sq_recv.at[l, h], sq_rs.at[l, h])
            total = jnp.zeros((8, LANES), f32)
            for r in range(n):
                total = total + sq_recv[l, h, r]
            inverse = lax.rsqrt(total / width + EPS)
            scale[...] = jnp.broadcast_to(inverse[0:1], (LANES, LANES)).T[0:rows]

        def split(i):
            at = jnp.maximum(i, 0)
            l = at // period
            rest = at - l * period
            valid = (i >= 0) & (l < layers) & (rest < items)
            l = jnp.minimum(l, layers - 1)
            rest = jnp.minimum(rest, items - 1)
            h = rest // chunks
            return valid, l, h, rest - h * chunks

        def later(i):
            last = (layers - 1) * period
            return jnp.where(i < last, i, jnp.where(i < last + LAST_BACK, -1, i - LAST_BACK))

        def step(t, carry):
            for lane in range(2):
                k = place(lane)
                valid, l, h, c = split(t - SKEW * (k - 1))

                @pl.when(valid & (k > 0))
                def _():
                    arrived(rs_recv.at[l, h, lane, 0:3], rs_rs.at[h, lane, c])

                    @pl.when(k < n - 1)
                    def _():
                        rs_send[l, h, lane, c] = (part[h, lane, c] + rs_recv[l, h, lane, c].astype(f32)).astype(bf16)
                        rs_copy(l, h, lane, c).start()

                    @pl.when(k == n - 1)
                    def _():
                        @pl.when(c == 0)
                        def _():
                            finish_scale(l, h)

                        factor = jnp.concatenate([scale[...]] * (cw // LANES), axis=1)
                        rest = coef[l, c]
                        gate = (part[h, lane, c, :, :cw] + rs_recv[l, h, lane, c, :, :cw].astype(f32)) * factor
                        value = (part[h, lane, c, :, cw:] + rs_recv[l, h, lane, c, :, cw:].astype(f32)) * factor
                        gate = mix(gate, rest, 0)
                        value = mix(value, rest, taps + 1)
                        hid[l, h, lane, c] = (jax.nn.gelu(gate) * value).astype(bf16)
                        ag_copy(l, h, lane, c).start()

            for lane in range(2):
                k = place(lane)
                valid, l, h, c = split(later(t - off_owner - SKEW_BACK * (n - 1 - k)))

                @pl.when(valid & (k < n - 1))
                def _():
                    ag_copy(l, h, lane, c).wait_recv()

                    @pl.when(k > 0)
                    def _():
                        ag_copy(l, h, lane, c).start()

            i = jnp.maximum(later(t - off_own), 0)
            l = i // period
            rest = i - l * period
            tardy = jnp.where(l < layers - 1, OWN_EXTRA, 0)
            fires = jnp.where(
                rest < items - 1, lax.rem(rest, chunks) == chunks - 1, rest == items - 1 + tardy
            )
            h = jnp.minimum(rest // chunks, groups - 1)

            @pl.when(fires & (l < layers))
            def _():
                mine = own(mc)

                @pl.when((l == 0) & (h < half))
                def _():
                    mine_copy(h).wait_recv()

                arrived(rbuf.at[l, h, 1:m], t_rs.at[l, h])
                total = tbuf[l, h, mine].astype(f32)
                for o in range(1, m):
                    total = total + rbuf[l, h, o].astype(f32)
                new = (0.5 * snew[l, h, mine].astype(f32) + total).astype(bf16)

                @pl.when(l < layers - 1)
                def _():
                    snew[l + 1, h, mine] = new
                    for o in range(m):
                        n_copy(l + 1, h, o).start()

                @pl.when(l == layers - 1)
                def _():
                    fin[h] = new
                    for o in range(1, m):
                        f_copy(h, o).start()
                    values = new.astype(f32)
                    square = jnp.sum(values * values, axis=1, keepdims=True)
                    square = jnp.broadcast_to(jnp.concatenate([square] * (LANES // rq), axis=0), (LANES, LANES))
                    fsq_send[h] = square.T[0:1]

                    @pl.when(h < half)
                    def _():
                        f_copy(h, 0).start()
                        fsq_copy(h, 0, 0).start()

                    @pl.when(h >= half)
                    def _():
                        raw[h - half, mine] = new
                        fsq_recv[h - half, me * m + mc] = fsq_send[h]

                    for o in range(1, m):
                        fsq_copy(h, 0, o).start()

                    def spread(r, carry):
                        for o in range(m):
                            fsq_copy(h, r, o).start()
                        return carry

                    lax.fori_loop(1, n, spread, 0)

            valid, l, h, c = split(later(t - off_down))

            @pl.when(valid)
            def _():
                @pl.when(h == 0)
                def _():
                    pltpu.make_async_copy(dn.at[l, c], dn.at[l, c], dsem.at[l, c]).wait()

                acc[...] += jnp.dot(hid[l, h, 0, c], dn[l, c, 0], preferred_element_type=f32) + jnp.dot(
                    hid[l, h, 1, c], dn[l, c, 1], preferred_element_type=f32
                )

                @pl.when(c == chunks - 1)
                def _():
                    tbuf[l, h] = acc[...].astype(bf16)
                    for o in range(1, m):
                        t_copy(l, h, o).start()
                    acc[...] = jnp.zeros(acc.shape, f32)
                    for lane in range(2):
                        k = place(lane)

                        @pl.when((k > 0) & (k < n - 1))
                        def _():
                            left(rs_send.at[l, h, lane], rs_ss.at[l, h, lane])

                        @pl.when(k > 0)
                        def _():
                            left(hid.at[l, h, lane], ag_ss.at[l, h, lane])

            valid, l, h, c = split(later(t - off_end))

            @pl.when(valid & (c == chunks - 1) & (l == layers - 1) & (h >= half))
            def _():
                at = h - half
                arrived(raw.at[at, 0 : rows - rq], f_rs.at[h])
                arrived(fsq_recv.at[at, 1 : n * m], fs_rs.at[h])
                end(h)

            @pl.when(t == chunks - 1)
            def _():
                for x in range(1, layers):
                    for cc in range(chunks):
                        for lane in range(2):
                            dcopy(x, lane, cc).start()

            return carry

        lax.fori_loop(0, (layers - 1) * period + items + off_end + LAST_BACK, step, 0)

        for h in range(half, groups):
            full_copy(h).wait_send()
        for h in range(groups):
            for l in range(layers):
                left(tbuf.at[l, h, 0 : rows - rq], t_ss.at[l, h])
                if l:
                    left(snew.at[l, h], n_ss.at[l, h])
            home = h // half
            left(raw.at[0, 0 : rows - home * rq], f_ss.at[h])
            left(fsq_recv.at[0, home : n * m], fs_ss.at[h])


def body(n, m, width, stream, norm_gain, gate_weight, value_weight, gate_taps, value_taps,
         gate_bias, value_bias, down_weight, final_gain):
    batch, length, dl = stream.shape
    layers, _, ff = gate_weight.shape
    taps = gate_taps.shape[1]
    groups, rows = 2 * batch, length
    cw = UNITS
    chunks = ff // 2 // cw
    rq = rows // m
    bf16, f32 = jnp.bfloat16, jnp.float32
    vmem = pl.BlockSpec(memory_space=pltpu.VMEM)
    hbm = pl.BlockSpec(memory_space=pl.ANY)
    dma = pltpu.SemaphoreType.DMA
    pieces = (layers, groups, 2, chunks)
    result = pl.pallas_call(
        functools.partial(chain_kernel, (n, m, width)),
        out_shape=jax.ShapeDtypeStruct((batch * length, dl), bf16),
        in_specs=[vmem] * 7 + [hbm] * 3,
        out_specs=vmem,
        scratch_shapes=[
            pltpu.VMEM((layers, chunks, 2, dl, 2 * cw), bf16),
            pltpu.VMEM((layers, chunks, 2, cw, dl), bf16),
            pltpu.VMEM((rows, dl), bf16),
            pltpu.VMEM((groups, 2, chunks, rows, 2 * cw), f32),
            pltpu.VMEM(pieces + (rows, 2 * cw), bf16),
            pltpu.VMEM(pieces + (rows, 2 * cw), bf16),
            pltpu.VMEM(pieces + (rows, cw), bf16),
            pltpu.VMEM((rows, dl), f32),
            pltpu.VMEM((rows, LANES), f32),
            pltpu.VMEM((layers, chunks, -(-(2 * taps + 2) // 8) * 8, cw), f32),
            pltpu.VMEM((layers, groups, 8, LANES), f32),
            pltpu.VMEM((layers, groups, n, 8, LANES), f32),
            pltpu.VMEM((layers, groups, rows, dl), bf16),
            pltpu.VMEM((layers, groups, m, rq, dl), bf16),
            pltpu.VMEM((layers, groups, rows, dl), bf16),
            pltpu.VMEM((groups, rq, dl), bf16),
            pltpu.VMEM((groups // 2, rows, dl), bf16),
            pltpu.VMEM((groups, 1, LANES), f32),
            pltpu.VMEM((groups // 2, n * m, 1, LANES), f32),
            dma((layers, chunks)),
            dma((layers, chunks)),
            dma(pieces[:3]), dma(pieces[:3]), dma(pieces[1:]), dma(pieces[:3]), dma(pieces[1:]),
            dma((layers, groups, 2)), dma((layers, groups)),
            dma((layers, groups)), dma((layers, groups)),
            dma((layers, groups)), dma((layers, groups)),
            dma((groups,)), dma((groups,)),
            dma((groups,)), dma((groups,)),
            dma((groups,)), dma((groups,)),
        ],
        compiler_params=pltpu.CompilerParams(
            collective_id=0, has_side_effects=True, vmem_limit_bytes=67_000_000
        ),
    )(
        stream.reshape(batch * length, dl), norm_gain, gate_taps.swapaxes(0, 1), value_taps.swapaxes(0, 1),
        gate_bias, value_bias, final_gain, gate_weight, value_weight, down_weight,
    )
    return result.reshape(batch, length, dl)


def solution(mesh):
    n, m = mesh.shape["ra"], mesh.shape["cb"]

    def run(stream, *rest):
        specs = (
            P("dp", None, "ra"),
            P(None, "ra"),
            P(None, "ra", "cb"),
            P(None, "ra", "cb"),
            P(None, None, "cb"),
            P(None, None, "cb"),
            P(None, "cb"),
            P(None, "cb"),
            P(None, "cb", "ra"),
            P("ra"),
        )
        return jax.shard_map(
            functools.partial(body, n, m, stream.shape[2]),
            mesh=mesh, in_specs=specs, out_specs=P("dp", None, "ra"), check_vma=False,
        )(stream, *rest)

    return run
```

```python
import functools

import jax
import jax.numpy as jnp
from jax import lax
from jax.experimental import pallas as pl
from jax.experimental.pallas import tpu as pltpu
from jax.sharding import PartitionSpec as P

EPS = 1e-06
MESH = pl.DeviceIdType.MESH
LANES = 128
UNITS = 256
SKEW = 3
SKEW_BACK = 3
OWN_LAG = 3
NEXT_LAG = 7
TUNED_FOR = (4, 6)
SUMS = [0, 6, 13, 20, 31, 37, 44, 50]
BACKS = [6, 13, 19, 25, 37, 43, 51, 57]
OWNS = [24, 30, 36, 42, 59, 68, 72, 73]
UP, MIX = 0, 1


def chain_kernel(
    dims,
    *refs,
):
    ins, (out, s_in, ng, gt, vt, gb, vb, fg), rest = refs[:7], refs[10:18], refs[18:]
    (wg_hbm, wv_hbm, dn_hbm), held = refs[7:10], refs[11:18]
    return chain(dims, ins, held, wg_hbm, wv_hbm, dn_hbm, out, *rest)


def chain(
    dims, ins, held, wg_hbm, wv_hbm, dn_hbm,
    out,
    w, dn, u, part, rs_send, rs_recv, hid, acc, scale, coef,
    sq_send, sq_recv, tbuf, rbuf, snew, fin, raw, fsq_send, fsq_recv,
    wsem, dsem, xsem, p_ss, rs_ss, rs_rs, ag_ss, ag_rs, sq_ss, sq_rs,
    t_ss, t_rs, n_ss, n_rs, i_ss, i_rs, fs_ss, fs_rs, f_ss, f_rs,
):
    n, m, width = dims
    s_in, ng, gt, vt, gb, vb, fg = held
    layers, chunks, _, dl, cw2 = w.shape
    cw = cw2 // 2
    groups, rows = hid.shape[1], hid.shape[4]
    half = groups // 2
    rq = rows // m
    taps = gt.shape[0]
    me = lax.axis_index("ra")
    mc = lax.axis_index("cb")
    core = lax.axis_index("dp")
    f32, bf16 = jnp.float32, jnp.bfloat16
    items = groups * chunks
    off_owner = SKEW * (n - 2)
    off_down = off_owner + SKEW_BACK * (n - 1)
    period = max(items, chunks + off_down + OWN_LAG + NEXT_LAG)
    sums = [l * period + h * chunks for l in range(layers) for h in range(groups)]
    backs = [x + off_owner for x in sums]
    owns = [x + chunks - 1 + off_down + OWN_LAG for x in sums]
    if (n, chunks) == TUNED_FOR and len(sums) == len(SUMS):
        sums, backs, owns = SUMS, BACKS, OWNS
    begin = min(sums)
    finish = max(owns) + 1 + half

    def place(lane):
        return jnp.where(lane == 1, me, n - 1 - me)

    def wcopy(l, lane, c, which):
        src = (wg_hbm, wv_hbm)[which]
        cols = pl.ds(pl.multiple_of((lane * chunks + c) * cw, LANES), cw)
        return pltpu.make_async_copy(
            src.at[l, :, cols], w.at[l, c, lane, :, pl.ds(which * cw, cw)], wsem.at[jnp.where(l == 0, c, chunks + l - 1)]
        )

    def dcopy(l, lane, c):
        units = pl.ds(pl.multiple_of((lane * chunks + c) * cw, LANES), cw)
        return pltpu.make_async_copy(dn_hbm.at[l, units, :], dn.at[l, c, lane], dsem.at[l])

    def remote(src, dst, ss, rs, **to):
        return pltpu.make_async_remote_copy(
            src_ref=src, dst_ref=dst, send_sem=ss, recv_sem=rs, device_id=to, device_id_type=MESH
        )

    def toward(lane, back):
        step = jnp.where((lane == 1) != back, 1, n - 1)
        return lax.rem(me + step, n)

    def own(q):
        return pl.ds(pl.multiple_of(q * rq, rq), rq)

    def part_copy(l, h, lane, c):
        return remote(
            part.at[h, lane, c], part.at[h, lane, c], p_ss.at[h, lane], rs_rs.at[h, lane, c], dp=MIX
        )

    def rs_copy(l, h, lane, c):
        return remote(
            rs_send.at[l, h, lane, c], rs_recv.at[l, h, lane, c],
            rs_ss.at[h, lane], rs_rs.at[h, lane, c], ra=toward(lane, False), dp=MIX,
        )

    def ag_copy(l, h, lane, c):
        return remote(
            hid.at[l, h, lane, c], hid.at[l, h, lane, c],
            ag_ss.at[h, lane], ag_rs.at[h, lane, c], ra=toward(lane, True), dp=MIX,
        )

    def sq_copy(l, h, e):
        return remote(
            sq_send.at[l, h], sq_recv.at[l, h, me], sq_ss.at[h], sq_rs.at[h],
            ra=(0, n - 1)[e], dp=MIX,
        )

    def t_copy(l, h, o):
        to = lax.rem(mc + o, m)
        return remote(tbuf.at[l, h, own(to)], rbuf.at[l, h, o], t_ss.at[h], t_rs.at[h], cb=to)

    def n_copy(l, h, o):
        mine = own(mc)
        return remote(
            snew.at[l, h, mine], snew.at[l, h, mine], n_ss.at[h], n_rs.at[h],
            cb=lax.rem(mc + o, m), dp=UP,
        )

    def full_copy(h):
        return remote(
            s_in.at[pl.ds((h - half) * rows, rows)], snew.at[0, h], i_ss.at[0], i_rs.at[0], dp=UP
        )

    def mine_copy(h):
        return remote(
            s_in.at[pl.ds(pl.multiple_of(h * rows + mc * rq, rq), rq)], snew.at[0, h, own(mc)],
            i_ss.at[0], i_rs.at[0], dp=MIX,
        )

    def fsq_copy(h, r, o):
        return remote(
            fsq_send.at[h], fsq_recv.at[lax.rem(h, half), me * m + mc], fs_ss.at[h], fs_rs.at[h],
            ra=lax.rem(me + r, n), cb=lax.rem(mc + o, m), dp=h // half,
        )

    def f_copy(h, o):
        return remote(
            fin.at[h], raw.at[lax.rem(h, half), own(mc)], f_ss.at[h], f_rs.at[h],
            cb=lax.rem(mc + o, m), dp=h // half,
        )

    def arrived(ref, sem):
        remote(ref, ref, f_ss.at[0], sem, dp=core).wait_recv()

    def left(ref, sem):
        remote(ref, ref, sem, f_rs.at[0], dp=core).wait_send()

    def end(h):
        at = lax.rem(h, half)
        for q in range(m):
            total = fsq_recv[at, q]
            for r in range(1, n):
                total = total + fsq_recv[at, r * m + q]
            inverse = lax.rsqrt(total / width + EPS)
            factor = jnp.broadcast_to(inverse, (LANES, LANES)).T[0:rq]
            factor = jnp.concatenate([factor] * (dl // LANES), axis=1)
            scaled = raw[at, q * rq : (q + 1) * rq].astype(f32) * factor * fg[...].astype(f32).reshape(1, dl)
            out[pl.ds(pl.multiple_of(at * rows + q * rq, rq), rq)] = scaled.astype(bf16)

    barrier = pltpu.get_barrier_semaphore()

    def greet(**to):
        pl.semaphore_signal(barrier, inc=1, device_id=to, device_id_type=MESH)

    def fetch(x):
        return pltpu.make_async_copy(ins[x], held[x], xsem.at[x])

    near = 1 + jnp.where(me > 0, 1, 0) + jnp.where(me < n - 1, 1, 0)

    @pl.when(core == UP)
    def _():
        for o in range(m):
            greet(cb=lax.rem(mc + o, m), dp=MIX)
        for x in (0, 1, 6):
            fetch(x).start()
        for lane in range(2):
            for which in range(2):
                wcopy(0, lane, 0, which).start()

    @pl.when(core == MIX)
    def _():
        greet(dp=UP)

        @pl.when(me > 0)
        def _():
            greet(ra=me - 1, dp=UP)

        @pl.when(me < n - 1)
        def _():
            greet(ra=me + 1, dp=UP)

        for o in range(1, n):
            greet(ra=lax.rem(me + o, n), dp=MIX)
        for o in range(1, m):
            greet(cb=lax.rem(mc + o, m), dp=MIX)
        for x in (0, 2, 3, 4, 5, 6):
            fetch(x).start()

    @pl.when(core == UP)
    def _():
        for x in (0, 1, 6):
            fetch(x).wait()
        for c in range(1, chunks):
            for lane in range(2):
                for which in range(2):
                    wcopy(0, lane, c, which).start()
        for h in range(half):
            snew[0, h] = s_in[h * rows : (h + 1) * rows]

    @pl.when(core == MIX)
    def _():
        for x in (0, 2, 3, 4, 5, 6):
            fetch(x).wait()
        for c in range(chunks):
            for lane in range(2):
                dcopy(0, lane, c).start()
        mine = own(mc)
        for h in range(half, groups):
            snew[0, h, mine] = s_in[pl.ds(pl.multiple_of((h - half) * rows + mc * rq, rq), rq)]
        acc[...] = jnp.zeros(acc.shape, f32)
        lane = jnp.where(me == 0, 0, 1)
        for l in range(layers):
            for c in range(chunks):
                cols = pl.ds(pl.multiple_of((lane * chunks + c) * cw, LANES), cw)
                for i in range(taps):
                    coef[l, c, i : i + 1] = gt[i, l : l + 1, cols].astype(f32)
                    coef[l, c, taps + 1 + i : taps + 2 + i] = vt[i, l : l + 1, cols].astype(f32)
                coef[l, c, taps : taps + 1] = gb[l : l + 1, cols].astype(f32)
                coef[l, c, 2 * taps + 1 : 2 * taps + 2] = vb[l : l + 1, cols].astype(f32)

    @pl.when(core == UP)
    def _():
        first = jnp.where(me == 0, 1, 0)

        def item(i, carry):
            l = i // items
            rest = i - l * items
            h = rest // chunks
            c = rest - h * chunks

            @pl.when(c == 0)
            def _():
                @pl.when(l > 0)
                def _():
                    arrived(snew.at[l, h], n_rs.at[h])

                gain = ng[0:1, :].astype(f32)
                for x in range(1, layers):
                    gain = jnp.where(l == x, ng[x : x + 1, :].astype(f32), gain)
                u[...] = (snew[l, h].astype(f32) * gain).astype(bf16)

            @pl.when(h == 0)
            def _():
                @pl.when(l == 0)
                def _():
                    pltpu.make_async_copy(w.at[0, c], w.at[0, c], wsem.at[c]).wait()

                @pl.when((l > 0) & (c == 0))
                def _():
                    pltpu.make_async_copy(w.at[l], w.at[l], wsem.at[chunks + l - 1]).wait()


            for a in range(2):
                lane = first if a == 0 else 1 - first
                k = place(lane)

                def up():
                    return jnp.dot(u[...], w[l, c, lane], preferred_element_type=f32)

                if a == 0:

                    @pl.when(k == 0)
                    def _():
                        @pl.when((l > 0) & (c == 0))
                        def _():
                            left(rs_send.at[0, h, lane], rs_ss.at[h, lane])

                        rs_send[l, h, lane, c] = up().astype(bf16)

                @pl.when(k > 0)
                def _():
                    @pl.when((l > 0) & (c == 0))
                    def _():
                        left(part.at[h, lane], p_ss.at[h, lane])

                    part[h, lane, c] = up()

                if a == 0:

                    @pl.when(i == 0)
                    def _():
                        pl.semaphore_wait(barrier, near)

                    @pl.when(k == 0)
                    def _():
                        rs_copy(l, h, lane, c).start()

                @pl.when(k > 0)
                def _():
                    part_copy(l, h, lane, c).start()

            @pl.when(i == 0)
            def _():
                for x in range(half):
                    mine_copy(x).start()

            @pl.when(i == chunks - 2)
            def _():
                arrived(snew.at[0, half:groups], i_rs.at[0])

            @pl.when(c == chunks - 2)
            def _():
                @pl.when(l > 0)
                def _():
                    left(sq_send.at[0:2, 0], sq_ss.at[h])

                values = snew[l, h].astype(f32)
                total = jnp.sum(values * values, axis=1, keepdims=True)
                square = jnp.broadcast_to(jnp.concatenate([total] * (LANES // rows), axis=0), (LANES, LANES))
                sq_send[l, h] = square.T[0:8]
                for e in range(2):
                    sq_copy(l, h, e).start()

            @pl.when(i == chunks - 1)
            def _():
                for x in range(1, layers):
                    for cc in range(chunks):
                        for lane in range(2):
                            for which in range(2):
                                wcopy(x, lane, cc, which).start()

            return carry

        lax.fori_loop(0, layers * items, item, 0)

        for h in range(groups):
            for lane in range(2):
                k = place(lane)

                @pl.when(k == 0)
                def _():
                    left(rs_send.at[0, h, lane], rs_ss.at[h, lane])

                @pl.when(k > 0)
                def _():
                    left(part.at[h, lane], p_ss.at[h, lane])

            left(sq_send.at[0:2, 0], sq_ss.at[h])
        left(raw.at[:, own(0)], i_ss.at[0])
        for h in range(half):
            arrived(raw.at[h], f_rs.at[h])
            arrived(fsq_recv.at[h], fs_rs.at[h])
            end(h)

    @pl.when(core == MIX)
    def _():
        pl.semaphore_wait(barrier, n - 1 + 2 * m - 1)
        for h in range(half, groups):
            full_copy(h).start()

        position = lax.broadcasted_iota(jnp.int32, (rows, cw), 0)

        def mix(x, rest, at):
            result = rest[at + taps : at + taps + 1] + x * rest[at + taps - 1 : at + taps]
            for back in range(1, taps):
                moved = jnp.where(position >= back, pltpu.roll(x, back, 0), 0.0)
                result = result + moved * rest[at + taps - 1 - back : at + taps - back]
            return result

        def finish_scale(l, h):
            arrived(sq_recv.at[l, h], sq_rs.at[h])
            total = jnp.zeros((8, LANES), f32)
            for r in range(n):
                total = total + sq_recv[l, h, r]
            inverse = lax.rsqrt(total / width + EPS)
            scale[...] = jnp.broadcast_to(inverse[0:1], (LANES, LANES)).T[0:rows]

        def split(starts, i):
            at = i * 0
            for g, start in enumerate(starts):
                inside = (i >= start) & (i < start + chunks)
                valid = inside if g == 0 else valid | inside
                at = jnp.where(inside, g * chunks + i - start, at)
            l = at // items
            rest = at - l * items
            h = rest // chunks
            return valid, l, h, rest - h * chunks

        def due(times, i):
            valid = i == times[0]
            at = i * 0
            for g, time in enumerate(times):
                valid = valid | (i == time)
                at = jnp.where(i == time, g, at)
            l = at // groups
            return valid, l, at - l * groups

        def step(t, carry):
            for lane in range(2):
                k = place(lane)
                valid, l, h, c = split(sums, t - SKEW * (k - 1))

                @pl.when(valid & (k > 0))
                def _():
                    arrived(rs_recv.at[l, h, lane, 0:3], rs_rs.at[h, lane, c])

                    @pl.when(k < n - 1)
                    def _():
                        rs_send[l, h, lane, c] = (part[h, lane, c] + rs_recv[l, h, lane, c].astype(f32)).astype(bf16)
                        rs_copy(l, h, lane, c).start()

                    @pl.when(k == n - 1)
                    def _():
                        @pl.when(c == 0)
                        def _():
                            finish_scale(l, h)

                        factor = jnp.concatenate([scale[...]] * (cw // LANES), axis=1)
                        rest = coef[l, c]
                        gate = (part[h, lane, c, :, :cw] + rs_recv[l, h, lane, c, :, :cw].astype(f32)) * factor
                        value = (part[h, lane, c, :, cw:] + rs_recv[l, h, lane, c, :, cw:].astype(f32)) * factor
                        gate = mix(gate, rest, 0)
                        value = mix(value, rest, taps + 1)
                        hid[l, h, lane, c] = (jax.nn.gelu(gate) * value).astype(bf16)
                        ag_copy(l, h, lane, c).start()

            for lane in range(2):
                k = place(lane)
                valid, l, h, c = split(backs, t - SKEW_BACK * (n - 1 - k))

                @pl.when(valid & (k < n - 1))
                def _():
                    ag_copy(l, h, lane, c).wait_recv()

                    @pl.when(k > 0)
                    def _():
                        ag_copy(l, h, lane, c).start()

            valid, l, h = due(owns, t)

            @pl.when(valid)
            def _():
                mine = own(mc)

                @pl.when((l == 0) & (h == 0))
                def _():
                    arrived(raw.at[:, own(0)], i_rs.at[0])

                arrived(rbuf.at[l, h, 1:m], t_rs.at[h])
                total = tbuf[l, h, mine].astype(f32)
                for o in range(1, m):
                    total = total + rbuf[l, h, o].astype(f32)
                new = (0.5 * snew[l, h, mine].astype(f32) + total).astype(bf16)

                @pl.when(l < layers - 1)
                def _():
                    @pl.when(l > 0)
                    def _():
                        left(snew.at[0, h], n_ss.at[h])

                    snew[l + 1, h, mine] = new
                    for o in range(m):
                        n_copy(l + 1, h, o).start()

                @pl.when(l == layers - 1)
                def _():
                    fin[h] = new
                    values = new.astype(f32)
                    square = jnp.sum(values * values, axis=1, keepdims=True)
                    square = jnp.broadcast_to(jnp.concatenate([square] * (LANES // rq), axis=0), (LANES, LANES))
                    fsq_send[h] = square.T[0:1]

                    def spread(r, carry):
                        for o in range(m):
                            fsq_copy(h, r, o).start()
                        return carry

                    lax.fori_loop(1, n, spread, 0)
                    for o in range(1, m):
                        fsq_copy(h, 0, o).start()
                    for o in range(1, m):
                        f_copy(h, o).start()

                    @pl.when(h < half)
                    def _():
                        f_copy(h, 0).start()
                        fsq_copy(h, 0, 0).start()

                    @pl.when(h >= half)
                    def _():
                        raw[h - half, mine] = new
                        fsq_recv[h - half, me * m + mc] = fsq_send[h]

            valid, l, h, c = split(backs, t - SKEW_BACK * (n - 1))

            @pl.when(valid)
            def _():
                @pl.when((h == 0) & (c == 0))
                def _():
                    pltpu.make_async_copy(dn.at[l], dn.at[l], dsem.at[l]).wait()

                acc[...] += jnp.dot(hid[l, h, 0, c], dn[l, c, 0], preferred_element_type=f32) + jnp.dot(
                    hid[l, h, 1, c], dn[l, c, 1], preferred_element_type=f32
                )

                @pl.when(c == chunks - 1)
                def _():
                    tbuf[l, h] = acc[...].astype(bf16)

                    @pl.when(l > 0)
                    def _():
                        left(tbuf.at[0, h, 0 : rows - rq], t_ss.at[h])

                    for o in range(1, m):
                        t_copy(l, h, o).start()
                    acc[...] = jnp.zeros(acc.shape, f32)
                    for lane in range(2):
                        k = place(lane)

                        @pl.when((k > 0) & (k < n - 1))
                        def _():
                            left(rs_send.at[l, h, lane], rs_ss.at[h, lane])

                        @pl.when(k > 0)
                        def _():
                            left(hid.at[l, h, lane], ag_ss.at[h, lane])

            @pl.when(t > max(owns))
            def _():
                h = half + t - max(owns) - 1
                at = h - half
                arrived(raw.at[at, 0 : rows - rq], f_rs.at[h])
                arrived(fsq_recv.at[at, 1 : n * m], fs_rs.at[h])
                end(h)

            @pl.when(t == begin + chunks - 1)
            def _():
                for x in range(1, layers):
                    for cc in range(chunks):
                        for lane in range(2):
                            dcopy(x, lane, cc).start()

            return carry

        lax.fori_loop(begin, finish, step, 0)

        left(raw, i_ss.at[0])
        for h in range(groups):
            left(tbuf.at[0, h, 0 : rows - rq], t_ss.at[h])
            if layers > 1:
                left(snew.at[0, h], n_ss.at[h])
            home = h // half
            left(raw.at[0, 0 : rows - home * rq], f_ss.at[h])
            left(fsq_recv.at[0, home : n * m], fs_ss.at[h])


def body(n, m, width, stream, norm_gain, gate_weight, value_weight, gate_taps, value_taps,
         gate_bias, value_bias, down_weight, final_gain):
    batch, length, dl = stream.shape
    layers, _, ff = gate_weight.shape
    taps = gate_taps.shape[1]
    groups, rows = 2 * batch, length
    cw = UNITS
    chunks = ff // 2 // cw
    rq = rows // m
    bf16, f32 = jnp.bfloat16, jnp.float32
    vmem = pl.BlockSpec(memory_space=pltpu.VMEM)
    hbm = pl.BlockSpec(memory_space=pl.ANY)
    dma = pltpu.SemaphoreType.DMA
    pieces = (layers, groups, 2, chunks)
    small = (
        stream.reshape(batch * length, dl), norm_gain, gate_taps.swapaxes(0, 1), value_taps.swapaxes(0, 1),
        gate_bias, value_bias, final_gain,
    )
    result = pl.pallas_call(
        functools.partial(chain_kernel, (n, m, width)),
        out_shape=jax.ShapeDtypeStruct((batch * length, dl), bf16),
        in_specs=[hbm] * 10,
        out_specs=vmem,
        scratch_shapes=[pltpu.VMEM(x.shape, bf16) for x in small] + [
            pltpu.VMEM((layers, chunks, 2, dl, 2 * cw), bf16),
            pltpu.VMEM((layers, chunks, 2, cw, dl), bf16),
            pltpu.VMEM((rows, dl), bf16),
            pltpu.VMEM((groups, 2, chunks, rows, 2 * cw), f32),
            pltpu.VMEM(pieces + (rows, 2 * cw), bf16),
            pltpu.VMEM(pieces + (rows, 2 * cw), bf16),
            pltpu.VMEM(pieces + (rows, cw), bf16),
            pltpu.VMEM((rows, dl), f32),
            pltpu.VMEM((rows, LANES), f32),
            pltpu.VMEM((layers, chunks, -(-(2 * taps + 2) // 8) * 8, cw), f32),
            pltpu.VMEM((layers, groups, 8, LANES), f32),
            pltpu.VMEM((layers, groups, n, 8, LANES), f32),
            pltpu.VMEM((layers, groups, rows, dl), bf16),
            pltpu.VMEM((layers, groups, m, rq, dl), bf16),
            pltpu.VMEM((layers, groups, rows, dl), bf16),
            pltpu.VMEM((groups, rq, dl), bf16),
            pltpu.VMEM((groups // 2, rows, dl), bf16),
            pltpu.VMEM((groups, 1, LANES), f32),
            pltpu.VMEM((groups // 2, n * m, 1, LANES), f32),
            dma((chunks + layers - 1,)), dma((layers,)), dma((7,)),
            dma((groups, 2)), dma((groups, 2)), dma(pieces[1:]), dma((groups, 2)), dma(pieces[1:]),
            dma((groups,)), dma((groups,)), dma((groups,)), dma((groups,)), dma((groups,)), dma((groups,)),
            dma((1,)), dma((1,)), dma((groups,)), dma((groups,)), dma((groups,)), dma((groups,)),
        ],
        compiler_params=pltpu.CompilerParams(
            collective_id=0, has_side_effects=True, vmem_limit_bytes=67_000_000
        ),
    )(
        *small, gate_weight, value_weight, down_weight,
    )
    return result.reshape(batch, length, dl)


def solution(mesh):
    n, m = mesh.shape["ra"], mesh.shape["cb"]

    def run(stream, *rest):
        specs = (
            P("dp", None, "ra"),
            P(None, "ra"),
            P(None, "ra", "cb"),
            P(None, "ra", "cb"),
            P(None, None, "cb"),
            P(None, None, "cb"),
            P(None, "cb"),
            P(None, "cb"),
            P(None, "cb", "ra"),
            P("ra"),
        )
        return jax.shard_map(
            functools.partial(body, n, m, stream.shape[2]),
            mesh=mesh, in_specs=specs, out_specs=P("dp", None, "ra"), check_vma=False,
        )(stream, *rest)

    return run
```

```python
import functools

import jax
import jax.numpy as jnp
from jax import lax
from jax.experimental import pallas as pl
from jax.experimental.pallas import tpu as pltpu
from jax.sharding import PartitionSpec as P

EPS = 1e-06
MESH = pl.DeviceIdType.MESH
LANES = 128
UNITS = 256
SKEW = 3
SKEW_BACK = 3
OWN_LAG = 3
NEXT_LAG = 7
TUNED_FOR = (4, 6)
SUMS = [0, 6, 13, 20, 31, 37, 44, 50]
BACKS = [6, 13, 19, 25, 36, 42, 49, 55]
OWNS = [24, 30, 36, 42, 59, 66, 70, 71]
UP, MIX = 0, 1


def chain_kernel(
    dims,
    *refs,
):
    ins, (out, s_in, ng, gt, vt, gb, vb, fg), rest = refs[:7], refs[10:18], refs[18:]
    (wg_hbm, wv_hbm, dn_hbm), held = refs[7:10], refs[11:18]
    return chain(dims, ins, held, wg_hbm, wv_hbm, dn_hbm, out, *rest)


def chain(
    dims, ins, held, wg_hbm, wv_hbm, dn_hbm,
    out,
    w, dn, u, part, rs_send, rs_recv, hid, acc, scale, coef,
    sq_send, sq_recv, tbuf, rbuf, snew, fin, raw, fsq_send, fsq_recv,
    wsem, dsem, xsem, p_ss, rs_ss, rs_rs, ag_ss, ag_rs, sq_ss, sq_rs,
    t_ss, t_rs, n_ss, n_rs, i_ss, i_rs, fs_ss, fs_rs, f_ss, f_rs,
):
    n, m, width = dims
    s_in, ng, gt, vt, gb, vb, fg = held
    layers, chunks, _, dl, cw2 = w.shape
    cw = cw2 // 2
    groups, rows = hid.shape[1], hid.shape[4]
    half = groups // 2
    rq = rows // m
    taps = gt.shape[0]
    me = lax.axis_index("ra")
    mc = lax.axis_index("cb")
    core = lax.axis_index("dp")
    f32, bf16 = jnp.float32, jnp.bfloat16
    items = groups * chunks
    off_owner = SKEW * (n - 2)
    off_down = off_owner + SKEW_BACK * (n - 1)
    period = max(items, chunks + off_down + OWN_LAG + NEXT_LAG)
    sums = [l * period + h * chunks for l in range(layers) for h in range(groups)]
    backs = [x + off_owner for x in sums]
    owns = [x + chunks - 1 + off_down + OWN_LAG for x in sums]
    if (n, chunks) == TUNED_FOR and len(sums) == len(SUMS):
        sums, backs, owns = SUMS, BACKS, OWNS
    begin = min(sums)
    finish = max(owns) + 1 + half

    def place(lane):
        return jnp.where(lane == 1, me, n - 1 - me)

    def wcopy(l, lane, c, which):
        src = (wg_hbm, wv_hbm)[which]
        cols = pl.ds(pl.multiple_of((lane * chunks + c) * cw, LANES), cw)
        return pltpu.make_async_copy(
            src.at[l, :, cols], w.at[l, c, lane, :, pl.ds(which * cw, cw)], wsem.at[jnp.where(l == 0, c, chunks + l - 1)]
        )

    def dcopy(l, lane, c):
        units = pl.ds(pl.multiple_of((lane * chunks + c) * cw, LANES), cw)
        return pltpu.make_async_copy(dn_hbm.at[l, units, :], dn.at[l, c, lane], dsem.at[l])

    def remote(src, dst, ss, rs, **to):
        return pltpu.make_async_remote_copy(
            src_ref=src, dst_ref=dst, send_sem=ss, recv_sem=rs, device_id=to, device_id_type=MESH
        )

    def toward(lane, back):
        step = jnp.where((lane == 1) != back, 1, n - 1)
        return lax.rem(me + step, n)

    def own(q):
        return pl.ds(pl.multiple_of(q * rq, rq), rq)

    def part_copy(l, h, lane, c):
        return remote(
            part.at[h, lane, c], part.at[h, lane, c], p_ss.at[h, lane], rs_rs.at[h, lane, c], dp=MIX
        )

    def rs_copy(l, h, lane, c):
        return remote(
            rs_send.at[l, h, lane, c], rs_recv.at[l, h, lane, c],
            rs_ss.at[h, lane], rs_rs.at[h, lane, c], ra=toward(lane, False), dp=MIX,
        )

    def ag_copy(l, h, lane, c):
        return remote(
            hid.at[l, h, lane, c], hid.at[l, h, lane, c],
            ag_ss.at[h, lane], ag_rs.at[h, lane, c], ra=toward(lane, True), dp=MIX,
        )

    def sq_copy(l, h, e):
        return remote(
            sq_send.at[l, h], sq_recv.at[l, h, me], sq_ss.at[h], sq_rs.at[h],
            ra=(0, n - 1)[e], dp=MIX,
        )

    def t_copy(l, h, o):
        to = lax.rem(mc + o, m)
        return remote(tbuf.at[l, h, own(to)], rbuf.at[l, h, o], t_ss.at[h], t_rs.at[h], cb=to)

    def n_copy(l, h, o):
        mine = own(mc)
        return remote(
            snew.at[l, h, mine], snew.at[l, h, mine], n_ss.at[h], n_rs.at[h],
            cb=lax.rem(mc + o, m), dp=UP,
        )

    def full_copy(h):
        return remote(
            s_in.at[pl.ds((h - half) * rows, rows)], snew.at[0, h], i_ss.at[0], i_rs.at[0], dp=UP
        )

    def mine_copy(h):
        return remote(
            s_in.at[pl.ds(pl.multiple_of(h * rows + mc * rq, rq), rq)], snew.at[0, h, own(mc)],
            i_ss.at[0], i_rs.at[0], dp=MIX,
        )

    def fsq_copy(h, r, o):
        return remote(
            fsq_send.at[h], fsq_recv.at[lax.rem(h, half), me * m + mc], fs_ss.at[h], fs_rs.at[h],
            ra=lax.rem(me + r, n), cb=lax.rem(mc + o, m), dp=h // half,
        )

    def f_copy(h, o):
        return remote(
            fin.at[h], raw.at[lax.rem(h, half), own(mc)], f_ss.at[h], f_rs.at[h],
            cb=lax.rem(mc + o, m), dp=h // half,
        )

    def arrived(ref, sem):
        remote(ref, ref, f_ss.at[0], sem, dp=core).wait_recv()

    def left(ref, sem):
        remote(ref, ref, sem, f_rs.at[0], dp=core).wait_send()

    def end(h):
        at = lax.rem(h, half)
        for q in range(m):
            total = fsq_recv[at, q]
            for r in range(1, n):
                total = total + fsq_recv[at, r * m + q]
            inverse = lax.rsqrt(total / width + EPS)
            factor = jnp.broadcast_to(inverse, (LANES, LANES)).T[0:rq]
            factor = jnp.concatenate([factor] * (dl // LANES), axis=1)
            scaled = raw[at, q * rq : (q + 1) * rq].astype(f32) * factor * fg[...].astype(f32).reshape(1, dl)
            out[pl.ds(pl.multiple_of(at * rows + q * rq, rq), rq)] = scaled.astype(bf16)

    barrier = pltpu.get_barrier_semaphore()

    def greet(**to):
        pl.semaphore_signal(barrier, inc=1, device_id=to, device_id_type=MESH)

    def fetch(x):
        return pltpu.make_async_copy(ins[x], held[x], xsem.at[x])

    near = 1 + jnp.where(me > 0, 1, 0) + jnp.where(me < n - 1, 1, 0)

    @pl.when(core == UP)
    def _():
        for o in range(m):
            greet(cb=lax.rem(mc + o, m), dp=MIX)
        for x in (0, 1, 6):
            fetch(x).start()
        for lane in range(2):
            for which in range(2):
                wcopy(0, lane, 0, which).start()

    @pl.when(core == MIX)
    def _():
        greet(dp=UP)

        @pl.when(me > 0)
        def _():
            greet(ra=me - 1, dp=UP)

        @pl.when(me < n - 1)
        def _():
            greet(ra=me + 1, dp=UP)

        for o in range(1, n):
            greet(ra=lax.rem(me + o, n), dp=MIX)
        for o in range(1, m):
            greet(cb=lax.rem(mc + o, m), dp=MIX)
        for x in (0, 2, 3, 4, 5, 6):
            fetch(x).start()

    @pl.when(core == UP)
    def _():
        for x in (0, 1, 6):
            fetch(x).wait()
        for c in range(1, chunks):
            for lane in range(2):
                for which in range(2):
                    wcopy(0, lane, c, which).start()
        for h in range(half):
            snew[0, h] = s_in[h * rows : (h + 1) * rows]

    @pl.when(core == MIX)
    def _():
        for x in (0, 2, 3, 4, 5, 6):
            fetch(x).wait()
        for c in range(chunks):
            for lane in range(2):
                dcopy(0, lane, c).start()
        mine = own(mc)
        for h in range(half, groups):
            snew[0, h, mine] = s_in[pl.ds(pl.multiple_of((h - half) * rows + mc * rq, rq), rq)]
        acc[...] = jnp.zeros(acc.shape, f32)
        lane = jnp.where(me == 0, 0, 1)
        for l in range(layers):
            for c in range(chunks):
                cols = pl.ds(pl.multiple_of((lane * chunks + c) * cw, LANES), cw)
                for i in range(taps):
                    coef[l, c, i : i + 1] = gt[i, l : l + 1, cols].astype(f32)
                    coef[l, c, taps + 1 + i : taps + 2 + i] = vt[i, l : l + 1, cols].astype(f32)
                coef[l, c, taps : taps + 1] = gb[l : l + 1, cols].astype(f32)
                coef[l, c, 2 * taps + 1 : 2 * taps + 2] = vb[l : l + 1, cols].astype(f32)

    @pl.when(core == UP)
    def _():
        first = jnp.where(me == 0, 1, 0)

        def item(i, carry):
            l = i // items
            rest = i - l * items
            h = rest // chunks
            c = rest - h * chunks

            @pl.when(c == 0)
            def _():
                @pl.when(l > 0)
                def _():
                    arrived(snew.at[l, h], n_rs.at[h])

                gain = ng[0:1, :].astype(f32)
                for x in range(1, layers):
                    gain = jnp.where(l == x, ng[x : x + 1, :].astype(f32), gain)
                u[...] = (snew[l, h].astype(f32) * gain).astype(bf16)

            @pl.when(h == 0)
            def _():
                @pl.when(l == 0)
                def _():
                    pltpu.make_async_copy(w.at[0, c], w.at[0, c], wsem.at[c]).wait()

                @pl.when((l > 0) & (c == 0))
                def _():
                    pltpu.make_async_copy(w.at[l], w.at[l], wsem.at[chunks + l - 1]).wait()


            for a in range(2):
                lane = first if a == 0 else 1 - first
                k = place(lane)

                def up():
                    return jnp.dot(u[...], w[l, c, lane], preferred_element_type=f32)

                if a == 0:

                    @pl.when(k == 0)
                    def _():
                        @pl.when((l > 0) & (c == 0))
                        def _():
                            left(rs_send.at[0, h, lane], rs_ss.at[h, lane])

                        rs_send[l, h, lane, c] = up().astype(bf16)

                @pl.when(k > 0)
                def _():
                    @pl.when((l > 0) & (c == 0))
                    def _():
                        left(part.at[h, lane], p_ss.at[h, lane])

                    part[h, lane, c] = up()

                if a == 0:

                    @pl.when(i == 0)
                    def _():
                        pl.semaphore_wait(barrier, near)

                    @pl.when(k == 0)
                    def _():
                        rs_copy(l, h, lane, c).start()

                @pl.when(k > 0)
                def _():
                    part_copy(l, h, lane, c).start()

            @pl.when(i == 0)
            def _():
                for x in range(half):
                    mine_copy(x).start()

            @pl.when(i == chunks - 2)
            def _():
                arrived(snew.at[0, half:groups], i_rs.at[0])

            @pl.when(c == chunks - 2)
            def _():
                @pl.when(l > 0)
                def _():
                    left(sq_send.at[0:2, 0], sq_ss.at[h])

                values = snew[l, h].astype(f32)
                total = jnp.sum(values * values, axis=1, keepdims=True)
                square = jnp.broadcast_to(jnp.concatenate([total] * (LANES // rows), axis=0), (LANES, LANES))
                sq_send[l, h] = square.T[0:8]
                for e in range(2):
                    sq_copy(l, h, e).start()

            @pl.when(i == chunks - 1)
            def _():
                for x in range(1, layers):
                    for cc in range(chunks):
                        for lane in range(2):
                            for which in range(2):
                                wcopy(x, lane, cc, which).start()

            return carry

        lax.fori_loop(0, layers * items, item, 0)

        for h in range(groups):
            for lane in range(2):
                k = place(lane)

                @pl.when(k == 0)
                def _():
                    left(rs_send.at[0, h, lane], rs_ss.at[h, lane])

                @pl.when(k > 0)
                def _():
                    left(part.at[h, lane], p_ss.at[h, lane])

            left(sq_send.at[0:2, 0], sq_ss.at[h])
        left(raw.at[:, own(0)], i_ss.at[0])
        for h in range(half):
            arrived(raw.at[h], f_rs.at[h])
            arrived(fsq_recv.at[h], fs_rs.at[h])
            end(h)

    @pl.when(core == MIX)
    def _():
        pl.semaphore_wait(barrier, n - 1 + 2 * m - 1)
        for h in range(half, groups):
            full_copy(h).start()

        position = lax.broadcasted_iota(jnp.int32, (rows, cw), 0)

        def mix(x, rest, at):
            result = rest[at + taps : at + taps + 1] + x * rest[at + taps - 1 : at + taps]
            for back in range(1, taps):
                moved = jnp.where(position >= back, pltpu.roll(x, back, 0), 0.0)
                result = result + moved * rest[at + taps - 1 - back : at + taps - back]
            return result

        def finish_scale(l, h):
            arrived(sq_recv.at[l, h], sq_rs.at[h])
            total = jnp.zeros((8, LANES), f32)
            for r in range(n):
                total = total + sq_recv[l, h, r]
            inverse = lax.rsqrt(total / width + EPS)
            scale[...] = jnp.broadcast_to(inverse[0:1], (LANES, LANES)).T[0:rows]

        def split(starts, i):
            at = i * 0
            for g, start in enumerate(starts):
                inside = (i >= start) & (i < start + chunks)
                valid = inside if g == 0 else valid | inside
                at = jnp.where(inside, g * chunks + i - start, at)
            l = at // items
            rest = at - l * items
            h = rest // chunks
            return valid, l, h, rest - h * chunks

        def due(times, i):
            valid = i == times[0]
            at = i * 0
            for g, time in enumerate(times):
                valid = valid | (i == time)
                at = jnp.where(i == time, g, at)
            l = at // groups
            return valid, l, at - l * groups

        def step(t, carry):
            for lane in range(2):
                k = place(lane)
                valid, l, h, c = split(sums, t - SKEW * (k - 1))

                @pl.when(valid & (k > 0))
                def _():
                    arrived(rs_recv.at[l, h, lane, 0:3], rs_rs.at[h, lane, c])

                    @pl.when(k < n - 1)
                    def _():
                        rs_send[l, h, lane, c] = (part[h, lane, c] + rs_recv[l, h, lane, c].astype(f32)).astype(bf16)
                        rs_copy(l, h, lane, c).start()

                    @pl.when(k == n - 1)
                    def _():
                        @pl.when(c == 0)
                        def _():
                            finish_scale(l, h)

                        factor = jnp.concatenate([scale[...]] * (cw // LANES), axis=1)
                        rest = coef[l, c]
                        gate = (part[h, lane, c, :, :cw] + rs_recv[l, h, lane, c, :, :cw].astype(f32)) * factor
                        value = (part[h, lane, c, :, cw:] + rs_recv[l, h, lane, c, :, cw:].astype(f32)) * factor
                        gate = mix(gate, rest, 0)
                        value = mix(value, rest, taps + 1)
                        hid[l, h, lane, c] = (jax.nn.gelu(gate) * value).astype(bf16)
                        ag_copy(l, h, lane, c).start()

            for lane in range(2):
                k = place(lane)
                valid, l, h, c = split(backs, t - SKEW_BACK * (n - 1 - k))

                @pl.when(valid & (k < n - 1))
                def _():
                    ag_copy(l, h, lane, c).wait_recv()

                    @pl.when(k > 0)
                    def _():
                        ag_copy(l, h, lane, c).start()

            valid, l, h = due(owns, t)

            @pl.when(valid)
            def _():
                mine = own(mc)

                @pl.when((l == 0) & (h == 0))
                def _():
                    arrived(raw.at[:, own(0)], i_rs.at[0])

                arrived(rbuf.at[l, h, 1:m], t_rs.at[h])
                total = tbuf[l, h, mine].astype(f32)
                for o in range(1, m):
                    total = total + rbuf[l, h, o].astype(f32)
                new = (0.5 * snew[l, h, mine].astype(f32) + total).astype(bf16)

                @pl.when(l < layers - 1)
                def _():
                    @pl.when(l > 0)
                    def _():
                        left(snew.at[0, h], n_ss.at[h])

                    snew[l + 1, h, mine] = new
                    for o in range(m):
                        n_copy(l + 1, h, o).start()

                @pl.when(l == layers - 1)
                def _():
                    fin[h] = new
                    values = new.astype(f32)
                    square = jnp.sum(values * values, axis=1, keepdims=True)
                    square = jnp.broadcast_to(jnp.concatenate([square] * (LANES // rq), axis=0), (LANES, LANES))
                    fsq_send[h] = square.T[0:1]

                    def spread(r, carry):
                        for o in range(m):
                            fsq_copy(h, r, o).start()
                        return carry

                    lax.fori_loop(1, n, spread, 0)
                    for o in range(1, m):
                        fsq_copy(h, 0, o).start()
                    for o in range(1, m):
                        f_copy(h, o).start()

                    @pl.when(h < half)
                    def _():
                        f_copy(h, 0).start()
                        fsq_copy(h, 0, 0).start()

                    @pl.when(h >= half)
                    def _():
                        raw[h - half, mine] = new
                        fsq_recv[h - half, me * m + mc] = fsq_send[h]

            valid, l, h, c = split(backs, t - SKEW_BACK * (n - 1))

            @pl.when(valid)
            def _():
                @pl.when((h == 0) & (c == 0))
                def _():
                    pltpu.make_async_copy(dn.at[l], dn.at[l], dsem.at[l]).wait()

                acc[...] += jnp.dot(hid[l, h, 0, c], dn[l, c, 0], preferred_element_type=f32) + jnp.dot(
                    hid[l, h, 1, c], dn[l, c, 1], preferred_element_type=f32
                )

                @pl.when(c == chunks - 1)
                def _():
                    tbuf[l, h] = acc[...].astype(bf16)

                    @pl.when(l > 0)
                    def _():
                        left(tbuf.at[0, h, 0 : rows - rq], t_ss.at[h])

                    for o in range(1, m):
                        t_copy(l, h, o).start()
                    acc[...] = jnp.zeros(acc.shape, f32)
                    for lane in range(2):
                        k = place(lane)

                        @pl.when((k > 0) & (k < n - 1))
                        def _():
                            left(rs_send.at[l, h, lane], rs_ss.at[h, lane])

                        @pl.when(k > 0)
                        def _():
                            left(hid.at[l, h, lane], ag_ss.at[h, lane])

            @pl.when(t > max(owns))
            def _():
                h = half + t - max(owns) - 1
                at = h - half
                arrived(raw.at[at, 0 : rows - rq], f_rs.at[h])
                arrived(fsq_recv.at[at, 1 : n * m], fs_rs.at[h])
                end(h)

            @pl.when(t == begin + chunks - 1)
            def _():
                for x in range(1, layers):
                    for cc in range(chunks):
                        for lane in range(2):
                            dcopy(x, lane, cc).start()

            return carry

        lax.fori_loop(begin, finish, step, 0)

        left(raw, i_ss.at[0])
        for h in range(groups):
            left(tbuf.at[0, h, 0 : rows - rq], t_ss.at[h])
            if layers > 1:
                left(snew.at[0, h], n_ss.at[h])
            home = h // half
            left(raw.at[0, 0 : rows - home * rq], f_ss.at[h])
            left(fsq_recv.at[0, home : n * m], fs_ss.at[h])


def body(n, m, width, stream, norm_gain, gate_weight, value_weight, gate_taps, value_taps,
         gate_bias, value_bias, down_weight, final_gain):
    batch, length, dl = stream.shape
    layers, _, ff = gate_weight.shape
    taps = gate_taps.shape[1]
    groups, rows = 2 * batch, length
    cw = UNITS
    chunks = ff // 2 // cw
    rq = rows // m
    bf16, f32 = jnp.bfloat16, jnp.float32
    vmem = pl.BlockSpec(memory_space=pltpu.VMEM)
    hbm = pl.BlockSpec(memory_space=pl.ANY)
    dma = pltpu.SemaphoreType.DMA
    pieces = (layers, groups, 2, chunks)
    small = (
        stream.reshape(batch * length, dl), norm_gain, gate_taps.swapaxes(0, 1), value_taps.swapaxes(0, 1),
        gate_bias, value_bias, final_gain,
    )
    result = pl.pallas_call(
        functools.partial(chain_kernel, (n, m, width)),
        out_shape=jax.ShapeDtypeStruct((batch * length, dl), bf16),
        in_specs=[hbm] * 10,
        out_specs=vmem,
        scratch_shapes=[pltpu.VMEM(x.shape, bf16) for x in small] + [
            pltpu.VMEM((layers, chunks, 2, dl, 2 * cw), bf16),
            pltpu.VMEM((layers, chunks, 2, cw, dl), bf16),
            pltpu.VMEM((rows, dl), bf16),
            pltpu.VMEM((groups, 2, chunks, rows, 2 * cw), f32),
            pltpu.VMEM(pieces + (rows, 2 * cw), bf16),
            pltpu.VMEM(pieces + (rows, 2 * cw), bf16),
            pltpu.VMEM(pieces + (rows, cw), bf16),
            pltpu.VMEM((rows, dl), f32),
            pltpu.VMEM((rows, LANES), f32),
            pltpu.VMEM((layers, chunks, -(-(2 * taps + 2) // 8) * 8, cw), f32),
            pltpu.VMEM((layers, groups, 8, LANES), f32),
            pltpu.VMEM((layers, groups, n, 8, LANES), f32),
            pltpu.VMEM((layers, groups, rows, dl), bf16),
            pltpu.VMEM((layers, groups, m, rq, dl), bf16),
            pltpu.VMEM((layers, groups, rows, dl), bf16),
            pltpu.VMEM((groups, rq, dl), bf16),
            pltpu.VMEM((groups // 2, rows, dl), bf16),
            pltpu.VMEM((groups, 1, LANES), f32),
            pltpu.VMEM((groups // 2, n * m, 1, LANES), f32),
            dma((chunks + layers - 1,)), dma((layers,)), dma((7,)),
            dma((groups, 2)), dma((groups, 2)), dma(pieces[1:]), dma((groups, 2)), dma(pieces[1:]),
            dma((groups,)), dma((groups,)), dma((groups,)), dma((groups,)), dma((groups,)), dma((groups,)),
            dma((1,)), dma((1,)), dma((groups,)), dma((groups,)), dma((groups,)), dma((groups,)),
        ],
        compiler_params=pltpu.CompilerParams(
            collective_id=0, has_side_effects=True, vmem_limit_bytes=67_000_000
        ),
    )(
        *small, gate_weight, value_weight, down_weight,
    )
    return result.reshape(batch, length, dl)


def solution(mesh):
    n, m = mesh.shape["ra"], mesh.shape["cb"]

    def run(stream, *rest):
        specs = (
            P("dp", None, "ra"),
            P(None, "ra"),
            P(None, "ra", "cb"),
            P(None, "ra", "cb"),
            P(None, None, "cb"),
            P(None, None, "cb"),
            P(None, "cb"),
            P(None, "cb"),
            P(None, "cb", "ra"),
            P("ra"),
        )
        return jax.shard_map(
            functools.partial(body, n, m, stream.shape[2]),
            mesh=mesh, in_specs=specs, out_specs=P("dp", None, "ra"), check_vma=False,
        )(stream, *rest)

    return run
```
